32 devices in a mesh: ep: 8 (over z, core), tp: 4 (over y, x).
Axes of the slice: x: 2, y: 2, z: 4, core: 2. Of those that a mesh axis runs over, the one named last changes fastest.
Arguments:
- tokens: bfloat16 [2048, 2048], P('ep'), may hold values from -6 to 6
- gate_proj: bfloat16 [8, 2048, 4096], P('ep', None, 'tp'), may hold values from -0.125 to 0.125
- up_proj: bfloat16 [8, 2048, 4096], P('ep', None, 'tp'), may hold values from -0.125 to 0.125
- down_proj: bfloat16 [8, 4096, 2048], P('ep', 'tp'), may hold values from -0.09375 to 0.09375
- side_input_weight: bfloat16 [2048, 1024], P(None, 'tp'), may hold values from -0.125 to 0.125
- dense_out: bfloat16 [1024, 2048], P(None, 'tp'), may hold values from -0.1875 to 0.1875
- dense_gate: bfloat16 [2048], replicated, may hold values from -0.125 to 0.125
- chosen_rows: int32 [8, 256], P(None, 'ep'), may hold values from 0 to 255, as said below
- choice_weights: float32 [8, 256], P(None, 'ep'), may hold values from 0.25 to 1
Outputs:
- mixed: bfloat16 [2048, 2048], P('ep', 'tp')
The draws below stay inside these ranges and needn't reach their ends.
Inputs may be any that keep to these rules, and one draw needn't show every extreme that they name: `chosen_rows`: for each expert and each block of 32 columns (one index of ep), the 32 rows are distinct rows of that index's 256 tokens; every expert reads exactly 32 tokens of every index.
All inputs are finite; a program needn't handle non-finite values.
Results may differ from the reference program's by a relative error of at most 0.015.
Values may be sent and summed in bfloat16 or wider, within the bound.
A program may use at most 64 MiB of HBM per device.

```python
import jax
import jax.numpy as jnp
from jax import lax

D = 2048
FF = 4096
DENSE_FF = 1024
TOK_DEV = 256
SLOT = 32
EXPERTS = 8
CAP = 256
TOKENS = 2048
N_TP = 4


def draw_chosen_rows(key, part):
    block_list = TOKENS // TOK_DEV
    keys = jax.random.split(jax.random.fold_in(key, 17), EXPERTS * block_list)
    orders = jax.vmap(lambda k: jax.random.permutation(k, TOK_DEV))(keys)
    picked = orders[:, :SLOT].astype(jnp.int32)
    return picked.reshape(EXPERTS, block_list * SLOT)


def level_of(stream_key, extent, shards, least, largest):
    def one(axis_at, parts):
        draws = jax.random.uniform(jax.random.fold_in(jax.random.fold_in(stream_key, 6), axis_at), (parts,), jnp.float32, least / len(shards), largest / len(shards))
        return jnp.repeat(jnp.exp(draws), extent[axis_at] // parts).reshape((-1,) + (1,) * (len(extent) - axis_at - 1))

    level = one(*shards[0])
    for cut in shards[1:]:
        level = level * one(*cut)
    return level


def gaussian(rng, dims, width, bound, cuts=(), dtype=jnp.bfloat16):
    factor_of = level_of(rng, dims, cuts, -0.22, 0.18) if cuts else 1.0
    values = jax.random.normal(rng, dims, jnp.float32) * width * factor_of
    return jnp.minimum(jnp.maximum(values, -bound), bound).astype(dtype)


def setup_inputs(seed: int = 0) -> dict:
    splits = jax.random.split(jax.random.key(seed), 10)
    return {
        "tokens": gaussian(splits[0], (TOKENS, D), 1.0, 6.0, ((0, 8),)),
        "gate_proj": gaussian(splits[1], (EXPERTS, D, FF), D ** -0.5, 0.125, ((0, 8), (2, 4))),
        "up_proj": gaussian(splits[2], (EXPERTS, D, FF), D ** -0.5, 0.125, ((0, 8), (2, 4))),
        "down_proj": gaussian(splits[3], (EXPERTS, FF, D), FF ** -0.5, 0.09375, ((0, 8), (1, 4))),
        "side_input_weight": gaussian(splits[4], (D, DENSE_FF), D ** -0.5, 0.125, ((1, 4),)),
        "dense_out": gaussian(splits[5], (DENSE_FF, D), DENSE_FF ** -0.5, 0.1875, ((1, 4),)),
        "dense_gate": gaussian(splits[6], (D,), D ** -0.5, 0.125),
        "chosen_rows": draw_chosen_rows(jax.random.fold_in(splits[9], 71), 0),
        "choice_weights": jnp.clip(0.25 + 0.75 * jax.random.uniform(splits[8], (EXPERTS, CAP), jnp.float32) ** level_of(splits[8], (EXPERTS, CAP), ((1, 8),), -0.2, 0.2), 0.25, 1.0),
    }


def reference(tokens, gate_proj, up_proj, down_proj, side_input_weight, dense_out, dense_gate, chosen_rows, choice_weights):
    token_id = ((jnp.arange(CAP) // SLOT) * TOK_DEV).astype(jnp.int32)[None, :] + chosen_rows.astype(jnp.int32)

    def one_expert(routed, inputs):
        w_gate, w_up, w_down, ids, weights = inputs
        picked = jnp.take(tokens, ids, axis=0)
        gate_val = jnp.dot(picked, w_gate, preferred_element_type=jnp.float32)
        up_val = jnp.dot(picked, w_up, preferred_element_type=jnp.float32)
        hidden = (jax.nn.silu(gate_val) * up_val).astype(jnp.bfloat16)
        block_list = hidden.reshape(CAP, N_TP, FF // N_TP).astype(jnp.float32)
        down_weight_blocks = w_down.reshape(N_TP, FF // N_TP, D).astype(jnp.float32)
        part = jnp.einsum('lyk,yka->yla', block_list, down_weight_blocks, precision=lax.Precision.HIGHEST)
        part = lax.optimization_barrier(part.astype(jnp.bfloat16)).astype(jnp.float32)
        expert_out = jnp.sum(part, axis=0).astype(jnp.bfloat16)
        routed = routed.at[ids].add(weights[:, None] * expert_out.astype(jnp.float32))
        return routed, None

    routed, _ = lax.scan(one_expert, jnp.zeros((TOKENS, D), jnp.float32),
                         (gate_proj, up_proj, down_proj, token_id, choice_weights))
    dense_hidden = jax.nn.silu(jnp.dot(tokens, side_input_weight, preferred_element_type=jnp.float32)).astype(jnp.bfloat16)
    dense_val = jnp.dot(dense_hidden, dense_out, preferred_element_type=jnp.float32)
    side_gate = jax.nn.sigmoid(jnp.dot(tokens, dense_gate, preferred_element_type=jnp.float32))
    return (routed + side_gate[:, None] * dense_val).astype(jnp.bfloat16)
```

```python
import functools

import jax
import jax.numpy as jnp
from jax import lax
from jax.experimental import pallas as pl
from jax.experimental.pallas import tpu as pltpu
from jax.sharding import PartitionSpec as P

MESH = pl.DeviceIdType.MESH
LANES = 128


def plain_per_device(
    tokens,
    gate_proj,
    up_proj,
    down_proj,
    side_input_weight,
    dense_out,
    dense_gate,
    chosen_rows,
    choice_weights,
):
    tok_rows = tokens.shape[0]
    width = tokens.shape[1] // lax.axis_size("tp")
    column_position = lax.axis_index("tp") * width
    own_cols = lax.dynamic_slice_in_dim(tokens, column_position, width, 1)
    expert_count, slot_rows = chosen_rows.shape
    capacity = expert_count * slot_rows
    picked = jnp.take(own_cols, chosen_rows.reshape(-1), axis=0).reshape(
        expert_count, slot_rows, width
    )
    arrived = lax.all_to_all(picked, "ep", split_axis=0, concat_axis=1, tiled=True).reshape(
        capacity, width
    )
    piece = lax.all_gather(arrived, "tp", axis=1, tiled=True)
    gate_val = jnp.dot(piece, gate_proj[0], preferred_element_type=jnp.float32)
    up_val = jnp.dot(piece, up_proj[0], preferred_element_type=jnp.float32)
    hidden = (jax.nn.silu(gate_val) * up_val).astype(jnp.bfloat16)
    summed = lax.psum_scatter(
        lax.dot_general(
            down_proj[0], hidden, (((0,), (1,)), ((), ())), preferred_element_type=jnp.float32
        ).astype(jnp.bfloat16),
        "tp",
        scatter_dimension=0,
        tiled=True,
    )
    returned = lax.all_to_all(summed, "ep", split_axis=1, concat_axis=1, tiled=True)
    hits = (
        chosen_rows.reshape(-1)[:, None] == jnp.arange(tok_rows, dtype=jnp.int32)[None, :]
    ).astype(jnp.bfloat16)
    scaled = returned.astype(jnp.float32) * choice_weights.reshape(-1)[None, :]
    high_part = scaled.astype(jnp.bfloat16)
    lower_half = (scaled - high_part.astype(jnp.float32)).astype(jnp.bfloat16)
    contract = (((0,), (1,)), ((), ()))
    routed = lax.dot_general(
        hits, high_part, contract, preferred_element_type=jnp.float32
    ) + lax.dot_general(hits, lower_half, contract, preferred_element_type=jnp.float32)
    dense_hidden = jax.nn.silu(
        jnp.dot(tokens, side_input_weight, preferred_element_type=jnp.float32)
    ).astype(jnp.bfloat16)
    dense_val = jnp.dot(
        lax.all_gather(dense_hidden, "tp", axis=1, tiled=True),
        dense_out,
        preferred_element_type=jnp.float32,
    )
    side_gate = jax.nn.sigmoid(jnp.dot(tokens, dense_gate, preferred_element_type=jnp.float32))
    return (routed + side_gate[:, None] * dense_val).astype(jnp.bfloat16)


def dot(a, b):
    return jnp.dot(a, b, preferred_element_type=jnp.float32)


def silu(v):
    return v / (1.0 + jnp.exp(-v))


def layer_kernel(
    slot,
    tok_hbm,
    gate_hbm,
    up_hbm,
    down_hbm,
    side_hbm,
    dout_hbm,
    dgate_hbm,
    rows_hbm,
    cw_hbm,
    out_ref,
    dgate_ref,
    rows_ref,
    cw_ref,
    tok,
    w_gate,
    w_up,
    w_down,
    w_side,
    w_dout,
    pick,
    xin,
    g_acc,
    u_acc,
    hid,
    comb,
    dhid,
    dense,
    part,
    d_in,
    rx,
    ry,
    pair,
    fin,
    back,
    load_sem,
    send_sem,
    far_sem,
    z_sem,
    ag_sem,
    dh_sem,
    rsd_sem,
    rsx_sem,
    rsy_sem,
    ret_sem,
):
    n_ep = rows_ref.shape[0]
    e = lax.axis_index("ep")
    p = lax.axis_index("tp")
    px = p + 1 - 2 * (p % 2)
    py = p + 2 - 4 * (p // 2)
    pd = px + 2 - 4 * (px // 2)
    z = e // 2
    core = e % 2
    partner = e + 1 - 2 * core
    upper = z // 2
    inner = (z + upper) % 2
    chips = [z, 3 - 3 * upper, 2 - upper, z + 1 - 2 * (z % 2)]
    width = out_ref.shape[1]
    tok_rows = tok.shape[0]
    side = w_side.shape[1]
    to_x, to_y = {"tp": px}, {"tp": py}
    f32, bf16 = jnp.float32, jnp.bfloat16
    scope = jax.named_scope

    barrier = pltpu.get_barrier_semaphore()
    for k in range(1, n_ep):
        pl.semaphore_signal(
            barrier, inc=1, device_id={"ep": (e + k) % n_ep}, device_id_type=MESH
        )
    for there in (to_x, to_y):
        pl.semaphore_signal(barrier, inc=1, device_id=there, device_id_type=MESH)

    loads = []
    for i, (src, dst) in enumerate(
        (
            (tok_hbm, tok),
            (side_hbm, w_side),
            (gate_hbm.at[0], w_gate),
            (up_hbm.at[0], w_up),
            (down_hbm.at[0], w_down),
            (dout_hbm, w_dout),
            (rows_hbm, rows_ref),
            (cw_hbm, cw_ref),
            (dgate_hbm, dgate_ref),
        )
    ):
        loads.append(pltpu.make_async_copy(src, dst, load_sem.at[i]))
    for i in (6, 0, 1, 7, 8, 2, 3, 4, 5):
        loads[i].start()

    def block(owner):
        return pl.ds(pl.multiple_of(owner * slot, slot), slot)

    def at(pos):
        return pl.ds(pos * slot, slot)

    def cols_of(q):
        return pl.ds(pl.multiple_of(q * width, width), width)

    sends = []

    def send(src, dst, sem, there):
        copy = pltpu.make_async_remote_copy(
            src_ref=src,
            dst_ref=dst,
            send_sem=send_sem.at[len(sends)],
            recv_sem=sem,
            device_id=there,
            device_id_type=MESH,
        )
        copy.start()
        sends.append(copy)

    def arrive(dst, sem):
        pltpu.make_async_remote_copy(
            src_ref=dst,
            dst_ref=dst,
            send_sem=send_sem.at[0],
            recv_sem=sem,
            device_id=to_x,
            device_id_type=MESH,
        ).wait_recv()

    with scope("hits"):
        loads[6].wait()
        rows_t = rows_ref[...].astype(f32).T
        lane = lax.broadcasted_iota(jnp.int32, (slot, tok_rows), 1).astype(f32)
        hits = jnp.concatenate(
            [jnp.where(rows_t[:, k : k + 1] == lane, 1.0, 0.0) for k in range(n_ep)], axis=0
        )
        chosen = hits.astype(bf16)
        loads[0].wait()
    with scope("pick"):
        for q in range(tok.shape[1] // width):
            cols = pl.ds(q * width, width)
            pick[:, cols] = dot(chosen, tok[:, cols]).astype(bf16)
    with scope("barrier"):
        pl.semaphore_wait(barrier, n_ep + 1)

    own, far = cols_of(p), cols_of(pd)

    def slot_of(pos):
        return pl.ds(pl.multiple_of(pos * slot, slot), slot)

    crossing = []
    for i, (g, c) in enumerate(((1, 0), (1, 1), (2, 0), (2, 1))):
        peer = 2 * chips[g] + c
        pos = 2 * (1 + inner) + core
        crossing.append(
            pltpu.make_async_remote_copy(
                src_ref=pick.at[block(peer), own],
                dst_ref=xin.at[slot_of(pos), own],
                send_sem=far_sem.at[i],
                recv_sem=z_sem.at[pos],
                device_id={"ep": peer},
                device_id_type=MESH,
            )
        )

    def far_sends():
        for copy in crossing:
            copy.start()

    pl.when(inner == 0)(far_sends)
    for c in range(2):
        peer = 2 * chips[3] + c
        pos = 6 + core
        send(pick.at[block(peer)], xin.at[slot_of(pos)], z_sem.at[pos], {"ep": peer})
    send(pick.at[block(partner)], xin.at[at(1)], z_sem.at[1], {"ep": partner})
    with scope("dhid"):
        loads[1].wait()
        dhid[p] = silu(dot(tok[...], w_side[...])).astype(bf16)
    send(dhid.at[p], dhid.at[p], dh_sem.at[0], to_x)
    send(dhid.at[p], dhid.at[p], dh_sem.at[1], to_y)
    xin[at(0), :] = pick[block(e), :]

    def combine_weights():
        loads[7].wait()
        cw_t = cw_ref[...].T
        weight = jnp.concatenate([cw_t[:, k : k + 1] for k in range(n_ep)], axis=0)
        both = (hits * weight).T
        high = both.astype(bf16)
        comb[0] = high
        comb[1] = (both - high.astype(f32)).astype(bf16)

    tile = 2 * LANES

    def gate_up_part(g):
        rows = pl.ds(2 * g * slot, 2 * slot)
        for n in range(hid.shape[1] // tile):
            cols = pl.ds(n * tile, tile)
            for acc, w in ((g_acc, w_gate), (u_acc, w_up)):
                total = dot(xin[rows, own], w[own, cols])
                for q in (px, py):
                    total += dot(xin[rows, cols_of(q)], w[cols_of(q), cols])
                acc[:, cols] = total

    def gate_up_rest(g):
        rows = pl.ds(2 * g * slot, 2 * slot)
        for n in range(hid.shape[1] // tile):
            cols = pl.ds(n * tile, tile)
            gate = g_acc[:, cols] + dot(xin[rows, far], w_gate[far, cols])
            up = u_acc[:, cols] + dot(xin[rows, far], w_up[far, cols])
            hid[rows, cols] = (silu(gate) * up).astype(bf16)

    def gate_up(g, count=1, tiles=None):
        rows = pl.ds(2 * g * slot, 2 * count * slot)
        for n in tiles or range(hid.shape[1] // tile):
            cols = pl.ds(n * tile, tile)
            gate = dot(xin[rows, :], w_gate[:, cols])
            up = dot(xin[rows, :], w_up[:, cols])
            hid[rows, cols] = (silu(gate) * up).astype(bf16)

    def down(g, count, *slots):
        rows = pl.ds(2 * g * slot, 2 * count * slot)
        for to in slots:
            q = (p, px, py, pd)[to]
            for n in range(width // tile):
                src = pl.ds(pl.multiple_of(q * width + n * tile, tile), tile)
                part[to, rows, pl.ds(n * tile, tile)] = dot(
                    hid[rows, :], w_down[:, src]
                ).astype(bf16)

    def spread(pos):
        ref = xin.at[at(pos), own]
        arrive(ref, z_sem.at[pos])
        send(ref, ref, ag_sem.at[0, pos], to_x)
        send(ref, ref, ag_sem.at[1, pos], to_y)

    def forward(pos):
        if pos % 2 == 0:
            ref = xin.at[at(pos), cols_of(px)]
            arrive(ref, ag_sem.at[0, pos])
            send(ref, ref, ag_sem.at[2, pos], to_y)
        else:
            ref = xin.at[at(pos), cols_of(py)]
            arrive(ref, ag_sem.at[1, pos])
            send(ref, ref, ag_sem.at[2, pos], to_x)

    def gathered_xy(g):
        even, odd = 2 * g, 2 * g + 1
        arrive(xin.at[at(odd), cols_of(px)], ag_sem.at[0, odd])
        arrive(xin.at[at(even), cols_of(py)], ag_sem.at[1, even])

    def gathered_d(g):
        for pos in (2 * g, 2 * g + 1):
            arrive(xin.at[at(pos), far], ag_sem.at[2, pos])

    def first(g):
        even, odd = at(2 * g), at(2 * g + 1)
        send(part.at[3, odd], d_in.at[odd], rsd_sem.at[2 * g + 1], to_x)
        send(part.at[3, even], d_in.at[even], rsd_sem.at[2 * g], to_y)

    def direct(g):
        even, odd = at(2 * g), at(2 * g + 1)
        send(part.at[1, odd], rx.at[odd], rsx_sem.at[2 * g + 1], to_x)
        send(part.at[2, even], ry.at[even], rsy_sem.at[2 * g], to_y)

    def joined(g):
        for pos, src, dst, sem, there in (
            (2 * g, 1, rx, rsx_sem, to_x),
            (2 * g + 1, 2, ry, rsy_sem, to_y),
        ):
            b = at(pos)
            arrive(d_in.at[b], rsd_sem.at[pos])
            pair[b, :] = (part[src, b, :].astype(f32) + d_in[b, :].astype(f32)).astype(bf16)
            send(pair.at[b], dst.at[b], sem.at[pos], there)

    def finish(g):
        for c in range(2):
            pos = 2 * g + c
            b = at(pos)
            arrive(rx.at[b], rsx_sem.at[pos])
            arrive(ry.at[b], rsy_sem.at[pos])
            total = (
                part[0, b, :].astype(f32) + rx[b, :].astype(f32) + ry[b, :].astype(f32)
            ).astype(bf16)
            if pos == 0:
                back[block(e), :] = total
            else:
                fin[b, :] = total
                owner = partner if g == 0 else 2 * chips[g] + c
                send(fin.at[b], back.at[block(e)], ret_sem.at[e], {"ep": owner})

    half = tok_rows // 2

    def dense_branch():
        arrive(dhid.at[pd, pl.ds(0, half)], dh_sem.at[2])
        arrive(dhid.at[pd, pl.ds(half, half)], dh_sem.at[3])
        loads[5].wait()
        loads[8].wait()
        total = dot(dhid[0], w_dout[pl.ds(0, side)])
        for q in range(1, dhid.shape[0]):
            total += dot(dhid[q], w_dout[pl.ds(q * side, side)])
        logit = jnp.sum(
            tok[...].astype(f32) * dgate_ref[...].reshape(1, tok.shape[1]).astype(f32),
            axis=1,
            keepdims=True,
        )
        dense[...] = total / (1.0 + jnp.exp(-logit))

    with scope("in0"):
        arrive(xin.at[at(1)], z_sem.at[1])
        loads[2].wait()
        loads[3].wait()
    n_tiles = hid.shape[1] // tile
    with scope("gu0a"):
        gate_up(0, 1, range(n_tiles // 2))
    pl.when(inner == 1)(far_sends)
    with scope("gu0b"):
        gate_up(0, 1, range(n_tiles // 2, n_tiles))
    with scope("down0"):
        loads[4].wait()
        down(0, 1, 3)
        first(0)
        down(0, 1, 1, 2)
        direct(0)
        down(0, 1, 0)
    with scope("spread1"):
        spread(2)
        spread(3)
    with scope("comb"):
        combine_weights()
    with scope("spread2"):
        spread(4)
        spread(5)
    with scope("join0"):
        joined(0)
    with scope("fwd1"):
        forward(2)
        forward(3)
    with scope("dh_fwd"):
        arrive(dhid.at[px], dh_sem.at[0])
        ref = dhid.at[px, pl.ds(0, half)]
        send(ref, ref, dh_sem.at[2], to_y)
        arrive(dhid.at[py], dh_sem.at[1])
        ref = dhid.at[py, pl.ds(half, half)]
        send(ref, ref, dh_sem.at[3], to_x)
    with scope("in1xy"):
        gathered_xy(1)
    with scope("gu1p"):
        gate_up_part(1)
    with scope("fwd2"):
        forward(4)
        forward(5)
    with scope("in1d"):
        gathered_d(1)
    with scope("gu1r"):
        gate_up_rest(1)
    with scope("down1"):
        down(1, 1, 3)
        first(1)
        down(1, 1, 1, 2)
        direct(1)
        down(1, 1, 0)
    with scope("in3"):
        arrive(xin.at[at(6)], z_sem.at[6])
        arrive(xin.at[at(7)], z_sem.at[7])
    with scope("in2"):
        gathered_xy(2)
        gathered_d(2)
    with scope("gu2"):
        gate_up(2, 2)
    with scope("join1"):
        joined(1)
    with scope("down2"):
        down(2, 2, 3)
        first(2)
        first(3)
        down(2, 2, 1, 2)
        direct(2)
        direct(3)
        down(2, 2, 0)
    with scope("fin1"):
        finish(1)
    with scope("dense"):
        dense_branch()
    with scope("join2"):
        joined(2)
    with scope("join3"):
        joined(3)
    with scope("fin0"):
        finish(0)
    with scope("fin2"):
        finish(2)
    with scope("fin3"):
        finish(3)
    with scope("ret"):
        for k in range(1, n_ep):
            owner = (e + n_ep - k) % n_ep
            arrive(back.at[block(owner)], ret_sem.at[owner])
    with scope("out"):
        out_ref[...] = dense[...] + dot(comb[0], back[...]) + dot(comb[1], back[...])
    with scope("drain"):
        for copy in sends + crossing:
            copy.wait_send()


def fused_per_device(
    tokens,
    gate_proj,
    up_proj,
    down_proj,
    side_input_weight,
    dense_out,
    dense_gate,
    chosen_rows,
    choice_weights,
):
    n_ep, slot = chosen_rows.shape
    n_tp = lax.axis_size("tp")
    tok_rows, d = tokens.shape
    width = d // n_tp
    ff = gate_proj.shape[2]
    side = side_input_weight.shape[1]
    cap = n_ep * slot
    bf16, f32 = jnp.bfloat16, jnp.float32
    n_sends = 2 + 1 + 4 + 8 + 4 + 3 * n_ep + n_ep - 1
    hbm = pl.BlockSpec(memory_space=pltpu.HBM)
    vmem = pl.BlockSpec(memory_space=pltpu.VMEM)
    return pl.pallas_call(
        functools.partial(layer_kernel, slot),
        out_shape=pltpu.VMEM((tok_rows, width), f32),
        in_specs=[hbm] * 9,
        out_specs=vmem,
        scratch_shapes=[
            pltpu.VMEM(dense_gate.shape, bf16),
            pltpu.VMEM(chosen_rows.shape, jnp.int32),
            pltpu.VMEM(choice_weights.shape, f32),
            pltpu.VMEM((tok_rows, d), bf16),
            pltpu.VMEM((d, ff), bf16),
            pltpu.VMEM((d, ff), bf16),
            pltpu.VMEM((ff, d), bf16),
            pltpu.VMEM((d, side), bf16),
            pltpu.VMEM((n_tp * side, width), bf16),
            pltpu.VMEM((cap, d), bf16),
            pltpu.VMEM((cap, d), bf16),
            pltpu.VMEM((2 * slot, ff), f32),
            pltpu.VMEM((2 * slot, ff), f32),
            pltpu.VMEM((cap, ff), bf16),
            pltpu.VMEM((2, tok_rows, cap), bf16),
            pltpu.VMEM((n_tp, tok_rows, side), bf16),
            pltpu.VMEM((tok_rows, width), f32),
            pltpu.VMEM((4, cap, width), bf16),
            pltpu.VMEM((cap, width), bf16),
            pltpu.VMEM((cap, width), bf16),
            pltpu.VMEM((cap, width), bf16),
            pltpu.VMEM((cap, width), bf16),
            pltpu.VMEM((cap, width), bf16),
            pltpu.VMEM((cap, width), bf16),
            pltpu.SemaphoreType.DMA((9,)),
            pltpu.SemaphoreType.DMA((n_sends,)),
            pltpu.SemaphoreType.DMA((4,)),
            pltpu.SemaphoreType.DMA((n_ep,)),
            pltpu.SemaphoreType.DMA((3, n_ep)),
            pltpu.SemaphoreType.DMA((4,)),
            pltpu.SemaphoreType.DMA((n_ep,)),
            pltpu.SemaphoreType.DMA((n_ep,)),
            pltpu.SemaphoreType.DMA((n_ep,)),
            pltpu.SemaphoreType.DMA((n_ep,)),
        ],
        compiler_params=pltpu.CompilerParams(collective_id=0, has_side_effects=True),
    )(
        tokens,
        gate_proj,
        up_proj,
        down_proj,
        side_input_weight,
        dense_out,
        dense_gate,
        chosen_rows,
        choice_weights,
    ).astype(bf16)


def per_device(*args):
    tokens, gate_proj, chosen_rows = args[0], args[1], args[7]
    n_ep, slot = chosen_rows.shape
    n_tp = lax.axis_size("tp")
    width, tile = tokens.shape[1] // n_tp, 2 * LANES
    fits = (
        n_tp == 4
        and n_ep == 8
        and tokens.shape[0] == n_ep * slot
        and slot % 16 == 0
        and width % tile == 0
        and gate_proj.shape[2] % tile == 0
        and args[4].shape[1] % LANES == 0
    )
    return fused_per_device(*args) if fits else plain_per_device(*args)


def solution(mesh):
    placed = (
        P("ep", None),
        P("ep", None, "tp"),
        P("ep", None, "tp"),
        P("ep", "tp", None),
        P(None, "tp"),
        P(None, "tp"),
        P(),
        P(None, "ep"),
        P(None, "ep"),
    )
    return jax.shard_map(
        per_device, mesh=mesh, in_specs=placed, out_specs=P("ep", "tp"), check_vma=False
    )
```

```python
import functools

import jax
import jax.numpy as jnp
from jax import lax
from jax.experimental import pallas as pl
from jax.experimental.pallas import tpu as pltpu
from jax.sharding import PartitionSpec as P

MESH = pl.DeviceIdType.MESH
LANES = 128


def plain_per_device(
    tokens,
    gate_proj,
    up_proj,
    down_proj,
    side_input_weight,
    dense_out,
    dense_gate,
    chosen_rows,
    choice_weights,
):
    tok_rows = tokens.shape[0]
    width = tokens.shape[1] // lax.axis_size("tp")
    column_position = lax.axis_index("tp") * width
    own_cols = lax.dynamic_slice_in_dim(tokens, column_position, width, 1)
    expert_count, slot_rows = chosen_rows.shape
    capacity = expert_count * slot_rows
    picked = jnp.take(own_cols, chosen_rows.reshape(-1), axis=0).reshape(
        expert_count, slot_rows, width
    )
    arrived = lax.all_to_all(picked, "ep", split_axis=0, concat_axis=1, tiled=True).reshape(
        capacity, width
    )
    piece = lax.all_gather(arrived, "tp", axis=1, tiled=True)
    gate_val = jnp.dot(piece, gate_proj[0], preferred_element_type=jnp.float32)
    up_val = jnp.dot(piece, up_proj[0], preferred_element_type=jnp.float32)
    hidden = (jax.nn.silu(gate_val) * up_val).astype(jnp.bfloat16)
    summed = lax.psum_scatter(
        lax.dot_general(
            down_proj[0], hidden, (((0,), (1,)), ((), ())), preferred_element_type=jnp.float32
        ).astype(jnp.bfloat16),
        "tp",
        scatter_dimension=0,
        tiled=True,
    )
    returned = lax.all_to_all(summed, "ep", split_axis=1, concat_axis=1, tiled=True)
    hits = (
        chosen_rows.reshape(-1)[:, None] == jnp.arange(tok_rows, dtype=jnp.int32)[None, :]
    ).astype(jnp.bfloat16)
    scaled = returned.astype(jnp.float32) * choice_weights.reshape(-1)[None, :]
    high_part = scaled.astype(jnp.bfloat16)
    lower_half = (scaled - high_part.astype(jnp.float32)).astype(jnp.bfloat16)
    contract = (((0,), (1,)), ((), ()))
    routed = lax.dot_general(
        hits, high_part, contract, preferred_element_type=jnp.float32
    ) + lax.dot_general(hits, lower_half, contract, preferred_element_type=jnp.float32)
    dense_hidden = jax.nn.silu(
        jnp.dot(tokens, side_input_weight, preferred_element_type=jnp.float32)
    ).astype(jnp.bfloat16)
    dense_val = jnp.dot(
        lax.all_gather(dense_hidden, "tp", axis=1, tiled=True),
        dense_out,
        preferred_element_type=jnp.float32,
    )
    side_gate = jax.nn.sigmoid(jnp.dot(tokens, dense_gate, preferred_element_type=jnp.float32))
    return (routed + side_gate[:, None] * dense_val).astype(jnp.bfloat16)


def dot(a, b):
    return jnp.dot(a, b, preferred_element_type=jnp.float32)


def silu(v):
    return v / (1.0 + jnp.exp(-v))


def layer_kernel(
    slot,
    tok_hbm,
    gate_hbm,
    up_hbm,
    down_hbm,
    side_hbm,
    dout_hbm,
    dgate_hbm,
    rows_hbm,
    cw_hbm,
    out_ref,
    dgate_ref,
    rows_ref,
    cw_ref,
    tok,
    w_gate,
    w_up,
    w_down,
    w_side,
    w_dout,
    pick,
    xin,
    g_acc,
    u_acc,
    hid,
    comb,
    dhid,
    dense,
    part,
    d_in,
    rx,
    ry,
    pair,
    fin,
    back,
    load_sem,
    send_sem,
    z_sem,
    ag_sem,
    dh_sem,
    rsd_sem,
    rsx_sem,
    rsy_sem,
    ret_sem,
):
    n_ep = rows_ref.shape[0]
    e = lax.axis_index("ep")
    p = lax.axis_index("tp")
    px = p + 1 - 2 * (p % 2)
    py = p + 2 - 4 * (p // 2)
    pd = px + 2 - 4 * (px // 2)
    z = e // 2
    core = e % 2
    partner = e + 1 - 2 * core
    upper = z // 2
    inner = (z + upper) % 2
    chips = [z, 3 - 3 * upper, 2 - upper, z + 1 - 2 * (z % 2)]
    near, late, mate = 1, 2, 3
    direct_in, direct_out = (), ()
    width = out_ref.shape[1]
    tok_rows = tok.shape[0]
    side = w_side.shape[1]
    to_x, to_y, to_d = {"tp": px}, {"tp": py}, {"tp": pd}
    f32, bf16 = jnp.float32, jnp.bfloat16
    scope = jax.named_scope

    def block(owner):
        return pl.ds(pl.multiple_of(owner * slot, slot), slot)

    def at(pos):
        return pl.ds(pos * slot, slot)

    def cols_of(q):
        return pl.ds(pl.multiple_of(q * width, width), width)

    own, far = cols_of(p), cols_of(pd)

    barrier = pltpu.get_barrier_semaphore()
    for k in range(1, n_ep):
        pl.semaphore_signal(
            barrier, inc=1, device_id={"ep": (e + k) % n_ep}, device_id_type=MESH
        )
    for there in (to_x, to_y, to_d):
        pl.semaphore_signal(barrier, inc=1, device_id=there, device_id_type=MESH)

    loads = []
    for i, (src, dst) in enumerate(
        (
            (tok_hbm.at[:, own], tok.at[:, own]),
            (side_hbm, w_side),
            (gate_hbm.at[0], w_gate),
            (up_hbm.at[0], w_up),
            (down_hbm.at[0], w_down),
            (dout_hbm, w_dout),
            (rows_hbm, rows_ref),
            (cw_hbm, cw_ref),
            (dgate_hbm, dgate_ref),
            *((tok_hbm.at[:, cols_of(q)], tok.at[:, cols_of(q)]) for q in (px, py, pd)),
        )
    ):
        loads.append(pltpu.make_async_copy(src, dst, load_sem.at[i]))
    for i in (6, 0, 9, 10, 11, 1, 7, 8, 2, 3, 4, 5):
        loads[i].start()

    sends = []

    def send(src, dst, sem, there):
        copy = pltpu.make_async_remote_copy(
            src_ref=src,
            dst_ref=dst,
            send_sem=send_sem.at[len(sends)],
            recv_sem=sem,
            device_id=there,
            device_id_type=MESH,
        )
        copy.start()
        sends.append(copy)

    def arrive(dst, sem):
        pltpu.make_async_remote_copy(
            src_ref=dst,
            dst_ref=dst,
            send_sem=send_sem.at[0],
            recv_sem=sem,
            device_id=to_x,
            device_id_type=MESH,
        ).wait_recv()

    with scope("hits"):
        loads[6].wait()
        rows_t = rows_ref[...].astype(f32).T
        lane = lax.broadcasted_iota(jnp.int32, (slot, tok_rows), 1).astype(f32)
        hits = jnp.concatenate(
            [jnp.where(rows_t[:, k : k + 1] == lane, 1.0, 0.0) for k in range(n_ep)], axis=0
        )
        chosen = hits.astype(bf16)
        loads[0].wait()
    with scope("pick"):
        pick[:, own] = dot(chosen, tok[:, own]).astype(bf16)
    with scope("barrier"):
        pl.semaphore_wait(barrier, n_ep + 2)

    def slot_of(pos):
        return pl.ds(pl.multiple_of(pos * slot, slot), slot)

    for g in (near, late):
        for c in range(2):
            peer = 2 * chips[g] + c
            pos = 2 * (near + inner) + core
            dst = xin.at[slot_of(pos), own]
            send(pick.at[block(peer), own], dst, z_sem.at[pos], {"ep": peer})
    with scope("pick2"):
        for i, q in enumerate((px, py, pd)):
            loads[9 + i].wait()
            pick[:, cols_of(q)] = dot(chosen, tok[:, cols_of(q)]).astype(bf16)
    send(pick.at[block(partner)], xin.at[at(1)], z_sem.at[1], {"ep": partner})
    for c in range(2):
        peer = 2 * chips[mate] + c
        pos = 2 * mate + core
        send(pick.at[block(peer)], xin.at[slot_of(pos)], z_sem.at[pos], {"ep": peer})
    with scope("dhid"):
        loads[1].wait()
        dhid[p] = silu(dot(tok[...], w_side[...])).astype(bf16)
    send(dhid.at[p], dhid.at[p], dh_sem.at[0], to_x)
    send(dhid.at[p], dhid.at[p], dh_sem.at[1], to_y)
    xin[at(0), :] = pick[block(e), :]

    def combine_weights():
        loads[7].wait()
        cw_t = cw_ref[...].T
        weight = jnp.concatenate([cw_t[:, k : k + 1] for k in range(n_ep)], axis=0)
        both = (hits * weight).T
        high = both.astype(bf16)
        comb[0] = high
        comb[1] = (both - high.astype(f32)).astype(bf16)

    tile = 2 * LANES

    def gate_up_part(g, count):
        rows = pl.ds(2 * g * slot, 2 * count * slot)
        for n in range(hid.shape[1] // tile):
            cols = pl.ds(n * tile, tile)
            for acc, w in ((g_acc, w_gate), (u_acc, w_up)):
                total = dot(xin[rows, own], w[own, cols])
                for q in (px, py):
                    total += dot(xin[rows, cols_of(q)], w[cols_of(q), cols])
                acc[rows, cols] = total

    def gate_up_rest(g, count):
        rows = pl.ds(2 * g * slot, 2 * count * slot)
        for n in range(hid.shape[1] // tile):
            cols = pl.ds(n * tile, tile)
            gate = g_acc[rows, cols] + dot(xin[rows, far], w_gate[far, cols])
            up = u_acc[rows, cols] + dot(xin[rows, far], w_up[far, cols])
            hid[rows, cols] = (silu(gate) * up).astype(bf16)

    def gate_up(g, count=1, tiles=None):
        rows = pl.ds(2 * g * slot, 2 * count * slot)
        for n in tiles or range(hid.shape[1] // tile):
            cols = pl.ds(n * tile, tile)
            gate = dot(xin[rows, :], w_gate[:, cols])
            up = dot(xin[rows, :], w_up[:, cols])
            hid[rows, cols] = (silu(gate) * up).astype(bf16)

    def down(g, count, *slots):
        rows = pl.ds(2 * g * slot, 2 * count * slot)
        for to in slots:
            q = (p, px, py, pd)[to]
            for n in range(width // tile):
                src = pl.ds(pl.multiple_of(q * width + n * tile, tile), tile)
                part[to, rows, pl.ds(n * tile, tile)] = dot(
                    hid[rows, :], w_down[:, src]
                ).astype(bf16)

    def spread(g):
        even, odd = 2 * g, 2 * g + 1
        for pos in (even, odd):
            arrive(xin.at[at(pos), own], z_sem.at[pos])
        order = ((even, 0), (odd, 1), (odd, 0), (even, 1))
        if g in direct_in:
            order = ((even, 2), (odd, 2)) + order
        for pos, axis in order:
            ref = xin.at[at(pos), own]
            send(ref, ref, ag_sem.at[axis, pos], (to_x, to_y, to_d)[axis])

    def forward(g):
        if g in direct_in:
            return
        even, odd = 2 * g, 2 * g + 1
        for pos, axis, q, there in ((even, 0, px, to_y), (odd, 1, py, to_x)):
            ref = xin.at[at(pos), cols_of(q)]
            arrive(ref, ag_sem.at[axis, pos])
            send(ref, ref, ag_sem.at[2, pos], there)

    def gathered_xy(g):
        even, odd = 2 * g, 2 * g + 1
        for pos in (even, odd):
            if g in direct_in or pos == odd:
                arrive(xin.at[at(pos), cols_of(px)], ag_sem.at[0, pos])
            if g in direct_in or pos == even:
                arrive(xin.at[at(pos), cols_of(py)], ag_sem.at[1, pos])

    def gathered_d(g):
        for pos in (2 * g, 2 * g + 1):
            arrive(xin.at[at(pos), far], ag_sem.at[2, pos])

    def first(g):
        for pos, there in ((2 * g + 1, to_x), (2 * g, to_y)):
            there = to_d if g in direct_out else there
            send(part.at[3, at(pos)], d_in.at[at(pos)], rsd_sem.at[pos], there)

    def direct(g):
        even, odd = 2 * g, 2 * g + 1
        for pos in (odd, even):
            b = at(pos)
            if g in direct_out or pos == odd:
                send(part.at[1, b], rx.at[b], rsx_sem.at[pos], to_x)
            if g in direct_out or pos == even:
                send(part.at[2, b], ry.at[b], rsy_sem.at[pos], to_y)

    def joined(g):
        if g in direct_out:
            return
        for pos, src, dst, sem, there in (
            (2 * g, 1, rx, rsx_sem, to_x),
            (2 * g + 1, 2, ry, rsy_sem, to_y),
        ):
            b = at(pos)
            arrive(d_in.at[b], rsd_sem.at[pos])
            pair[b, :] = (part[src, b, :].astype(f32) + d_in[b, :].astype(f32)).astype(bf16)
            send(pair.at[b], dst.at[b], sem.at[pos], there)

    def finish(g):
        for c in range(2):
            pos = 2 * g + c
            b = at(pos)
            arrive(rx.at[b], rsx_sem.at[pos])
            arrive(ry.at[b], rsy_sem.at[pos])
            total = part[0, b, :].astype(f32) + rx[b, :].astype(f32) + ry[b, :].astype(f32)
            if g in direct_out:
                arrive(d_in.at[b], rsd_sem.at[pos])
                total += d_in[b, :].astype(f32)
            if pos == 0:
                back[block(e), :] = total.astype(bf16)
            else:
                fin[b, :] = total.astype(bf16)
                owner = partner if g == 0 else 2 * chips[g] + c
                send(fin.at[b], back.at[block(e)], ret_sem.at[e], {"ep": owner})

    half = tok_rows // 2

    def dense_branch():
        arrive(dhid.at[pd, pl.ds(0, half)], dh_sem.at[2])
        arrive(dhid.at[pd, pl.ds(half, half)], dh_sem.at[3])
        loads[5].wait()
        loads[8].wait()
        total = dot(dhid[0], w_dout[pl.ds(0, side)])
        for q in range(1, dhid.shape[0]):
            total += dot(dhid[q], w_dout[pl.ds(q * side, side)])
        logit = jnp.sum(
            tok[...].astype(f32) * dgate_ref[...].reshape(1, tok.shape[1]).astype(f32),
            axis=1,
            keepdims=True,
        )
        dense[...] = total / (1.0 + jnp.exp(-logit))

    with scope("in0"):
        arrive(xin.at[at(1)], z_sem.at[1])
        loads[2].wait()
        loads[3].wait()
    n_tiles = hid.shape[1] // tile
    with scope("gu0a"):
        gate_up(0, 1, range(n_tiles // 2))
    with scope("gu0b"):
        gate_up(0, 1, range(n_tiles // 2, n_tiles))
    with scope("down0"):
        loads[4].wait()
        down(0, 1, 3)
        first(0)
        down(0, 1, 1, 2)
        direct(0)
        down(0, 1, 0)
    with scope("spreadA"):
        spread(near)
    with scope("comb"):
        combine_weights()
    with scope("spreadB"):
        spread(late)
    with scope("fwdA"):
        forward(near)
    with scope("join0"):
        joined(0)
    with scope("fwdB"):
        forward(late)
    with scope("dh_fwd"):
        arrive(dhid.at[px], dh_sem.at[0])
        ref = dhid.at[px, pl.ds(0, half)]
        send(ref, ref, dh_sem.at[2], to_y)
        arrive(dhid.at[py], dh_sem.at[1])
        ref = dhid.at[py, pl.ds(half, half)]
        send(ref, ref, dh_sem.at[3], to_x)
    with scope("inAxy"):
        gathered_xy(near)
    with scope("guAp"):
        gate_up_part(near, 1)
    with scope("inP"):
        for c in range(2):
            arrive(xin.at[at(2 * mate + c)], z_sem.at[2 * mate + c])
    with scope("inBxy"):
        gathered_xy(late)
    with scope("guBp"):
        gate_up_part(late, 2)
    with scope("inAd"):
        gathered_d(near)
    with scope("guAr"):
        gate_up_rest(near, 1)
    with scope("downA"):
        down(near, 1, 3)
        first(near)
        down(near, 1, 1, 2)
        direct(near)
    with scope("inBd"):
        gathered_d(late)
    with scope("guBr"):
        gate_up_rest(late, 2)
    with scope("downB"):
        down(late, 2, 3)
        first(mate)
        first(late)
        down(late, 2, 1, 2)
        down(near, 1, 0)
    with scope("joinA"):
        joined(near)
    direct(mate)
    with scope("downB0"):
        down(late, 2, 0)
    with scope("joinP"):
        joined(mate)
    direct(late)
    with scope("joinB"):
        joined(late)
    with scope("finA"):
        finish(near)
    with scope("fin0"):
        finish(0)
    with scope("finP"):
        finish(mate)
    with scope("finB"):
        finish(late)
    with scope("dense"):
        dense_branch()
    def returned(owner):
        arrive(back.at[block(owner)], ret_sem.at[owner])

    with scope("ret0"):
        returned(partner)
    for g in (near, mate, late):
        with scope(f"ret{'xABP'[g]}"):
            for c in range(2):
                returned(2 * chips[g] + c)
    with scope("out"):
        out_ref[...] = (
            dense[...] + dot(comb[0], back[...]) + dot(comb[1], back[...])
        ).astype(bf16)
    with scope("drain"):
        for copy in sends:
            copy.wait_send()


def fused_per_device(
    tokens,
    gate_proj,
    up_proj,
    down_proj,
    side_input_weight,
    dense_out,
    dense_gate,
    chosen_rows,
    choice_weights,
):
    n_ep, slot = chosen_rows.shape
    n_tp = lax.axis_size("tp")
    tok_rows, d = tokens.shape
    width = d // n_tp
    ff = gate_proj.shape[2]
    side = side_input_weight.shape[1]
    cap = n_ep * slot
    bf16, f32 = jnp.bfloat16, jnp.float32
    n_sends = (n_ep - 1) + 4 + 3 * (n_ep - 4) + 3 * n_ep + (n_ep - 1)
    hbm = pl.BlockSpec(memory_space=pltpu.HBM)
    vmem = pl.BlockSpec(memory_space=pltpu.VMEM)
    return pl.pallas_call(
        functools.partial(layer_kernel, slot),
        out_shape=pltpu.VMEM((tok_rows, width), bf16),
        in_specs=[hbm] * 9,
        out_specs=vmem,
        scratch_shapes=[
            pltpu.VMEM(dense_gate.shape, bf16),
            pltpu.VMEM(chosen_rows.shape, jnp.int32),
            pltpu.VMEM(choice_weights.shape, f32),
            pltpu.VMEM((tok_rows, d), bf16),
            pltpu.VMEM((d, ff), bf16),
            pltpu.VMEM((d, ff), bf16),
            pltpu.VMEM((ff, d), bf16),
            pltpu.VMEM((d, side), bf16),
            pltpu.VMEM((n_tp * side, width), bf16),
            pltpu.VMEM((cap, d), bf16),
            pltpu.VMEM((cap, d), bf16),
            pltpu.VMEM((cap, ff), f32),
            pltpu.VMEM((cap, ff), f32),
            pltpu.VMEM((cap, ff), bf16),
            pltpu.VMEM((2, tok_rows, cap), bf16),
            pltpu.VMEM((n_tp, tok_rows, side), bf16),
            pltpu.VMEM((tok_rows, width), f32),
            pltpu.VMEM((4, cap, width), bf16),
            pltpu.VMEM((cap, width), bf16),
            pltpu.VMEM((cap, width), bf16),
            pltpu.VMEM((cap, width), bf16),
            pltpu.VMEM((cap, width), bf16),
            pltpu.VMEM((cap, width), bf16),
            pltpu.VMEM((cap, width), bf16),
            pltpu.SemaphoreType.DMA((12,)),
            pltpu.SemaphoreType.DMA((n_sends,)),
            pltpu.SemaphoreType.DMA((n_ep,)),
            pltpu.SemaphoreType.DMA((3, n_ep)),
            pltpu.SemaphoreType.DMA((4,)),
            pltpu.SemaphoreType.DMA((n_ep,)),
            pltpu.SemaphoreType.DMA((n_ep,)),
            pltpu.SemaphoreType.DMA((n_ep,)),
            pltpu.SemaphoreType.DMA((n_ep,)),
        ],
        compiler_params=pltpu.CompilerParams(collective_id=0, has_side_effects=True),
    )(
        tokens,
        gate_proj,
        up_proj,
        down_proj,
        side_input_weight,
        dense_out,
        dense_gate,
        chosen_rows,
        choice_weights,
    )


def per_device(*args):
    tokens, gate_proj, chosen_rows = args[0], args[1], args[7]
    n_ep, slot = chosen_rows.shape
    n_tp = lax.axis_size("tp")
    width, tile = tokens.shape[1] // n_tp, 2 * LANES
    fits = (
        n_tp == 4
        and n_ep == 8
        and tokens.shape[0] == n_ep * slot
        and slot % 16 == 0
        and width % tile == 0
        and gate_proj.shape[2] % tile == 0
        and args[4].shape[1] % LANES == 0
    )
    return fused_per_device(*args) if fits else plain_per_device(*args)


def solution(mesh):
    placed = (
        P("ep", None),
        P("ep", None, "tp"),
        P("ep", None, "tp"),
        P("ep", "tp", None),
        P(None, "tp"),
        P(None, "tp"),
        P(),
        P(None, "ep"),
        P(None, "ep"),
    )
    return jax.shard_map(
        per_device, mesh=mesh, in_specs=placed, out_specs=P("ep", "tp"), check_vma=False
    )
```

```python
import functools
import math

import jax
import jax.numpy as jnp
from jax import lax
from jax.experimental import pallas as pl
from jax.experimental.pallas import tpu as pltpu
from jax.sharding import PartitionSpec as P

MESH = pl.DeviceIdType.MESH
LANES = 128


def plain_per_device(
    tokens,
    gate_proj,
    up_proj,
    down_proj,
    side_input_weight,
    dense_out,
    dense_gate,
    chosen_rows,
    choice_weights,
):
    tok_rows = tokens.shape[0]
    width = tokens.shape[1] // lax.axis_size("tp")
    column_position = lax.axis_index("tp") * width
    own_cols = lax.dynamic_slice_in_dim(tokens, column_position, width, 1)
    expert_count, slot_rows = chosen_rows.shape
    capacity = expert_count * slot_rows
    picked = jnp.take(own_cols, chosen_rows.reshape(-1), axis=0).reshape(
        expert_count, slot_rows, width
    )
    arrived = lax.all_to_all(picked, "ep", split_axis=0, concat_axis=1, tiled=True).reshape(
        capacity, width
    )
    piece = lax.all_gather(arrived, "tp", axis=1, tiled=True)
    gate_val = jnp.dot(piece, gate_proj[0], preferred_element_type=jnp.float32)
    up_val = jnp.dot(piece, up_proj[0], preferred_element_type=jnp.float32)
    hidden = (jax.nn.silu(gate_val) * up_val).astype(jnp.bfloat16)
    summed = lax.psum_scatter(
        lax.dot_general(
            down_proj[0], hidden, (((0,), (1,)), ((), ())), preferred_element_type=jnp.float32
        ).astype(jnp.bfloat16),
        "tp",
        scatter_dimension=0,
        tiled=True,
    )
    returned = lax.all_to_all(summed, "ep", split_axis=1, concat_axis=1, tiled=True)
    hits = (
        chosen_rows.reshape(-1)[:, None] == jnp.arange(tok_rows, dtype=jnp.int32)[None, :]
    ).astype(jnp.bfloat16)
    scaled = returned.astype(jnp.float32) * choice_weights.reshape(-1)[None, :]
    high_part = scaled.astype(jnp.bfloat16)
    lower_half = (scaled - high_part.astype(jnp.float32)).astype(jnp.bfloat16)
    contract = (((0,), (1,)), ((), ()))
    routed = lax.dot_general(
        hits, high_part, contract, preferred_element_type=jnp.float32
    ) + lax.dot_general(hits, lower_half, contract, preferred_element_type=jnp.float32)
    dense_hidden = jax.nn.silu(
        jnp.dot(tokens, side_input_weight, preferred_element_type=jnp.float32)
    ).astype(jnp.bfloat16)
    dense_val = jnp.dot(
        lax.all_gather(dense_hidden, "tp", axis=1, tiled=True),
        dense_out,
        preferred_element_type=jnp.float32,
    )
    side_gate = jax.nn.sigmoid(jnp.dot(tokens, dense_gate, preferred_element_type=jnp.float32))
    return (routed + side_gate[:, None] * dense_val).astype(jnp.bfloat16)


def dot(a, b):
    return jnp.dot(a, b, preferred_element_type=jnp.float32)


def silu(v):
    return v / (1.0 + jnp.exp(-v))


def layer_kernel(
    slot,
    tok_hbm,
    gate_hbm,
    up_hbm,
    down_hbm,
    side_hbm,
    dout_hbm,
    dgate_hbm,
    rows_hbm,
    cw_hbm,
    out_ref,
    dgate_ref,
    rows_ref,
    cw_ref,
    tok,
    w_gate,
    w_up,
    w_down,
    w_side,
    w_dout,
    pick,
    xin,
    g_acc,
    u_acc,
    hid,
    comb,
    dhid,
    dense,
    part,
    d_in,
    rx,
    ry,
    pair,
    fin,
    back,
    load_sem,
    send_sem,
    z_sem,
    ag_sem,
    dh_sem,
    d_sem,
    sum_sem,
    ret_sem,
):
    n_ep = rows_ref.shape[0]
    e = lax.axis_index("ep")
    p = lax.axis_index("tp")
    px = p + 1 - 2 * (p % 2)
    py = p + 2 - 4 * (p // 2)
    pd = px + 2 - 4 * (px // 2)
    z = e // 2
    core = e % 2
    partner = e + 1 - 2 * core
    upper = z // 2
    inner = (z + upper) % 2
    chips = [z, 3 - 3 * upper, 2 - upper, z + 1 - 2 * (z % 2)]
    near, late, mate = 1, 2, 3
    width = out_ref.shape[1]
    tok_rows = tok.shape[0]
    side = w_side.shape[1]
    to_x, to_y = {"tp": px}, {"tp": py}
    f32, bf16 = jnp.float32, jnp.bfloat16
    scope = jax.named_scope

    def block(owner):
        return pl.ds(pl.multiple_of(owner * slot, slot), slot)

    def at(pos):
        return pl.ds(pos * slot, slot)

    def cols_of(q):
        return pl.ds(pl.multiple_of(q * width, width), width)

    own, far = cols_of(p), cols_of(pd)

    barrier = pltpu.get_barrier_semaphore()
    for k in range(1, n_ep):
        pl.semaphore_signal(
            barrier, inc=1, device_id={"ep": (e + k) % n_ep}, device_id_type=MESH
        )
    for there in (to_x, to_y):
        pl.semaphore_signal(barrier, inc=1, device_id=there, device_id_type=MESH)

    loads = []
    for i, (src, dst) in enumerate(
        (
            (tok_hbm.at[:, own], tok.at[:, own]),
            (side_hbm, w_side),
            (gate_hbm.at[0], w_gate),
            (up_hbm.at[0], w_up),
            (down_hbm.at[0], w_down),
            (dout_hbm, w_dout),
            (rows_hbm, rows_ref),
            (cw_hbm, cw_ref),
            (dgate_hbm, dgate_ref),
            *((tok_hbm.at[:, cols_of(q)], tok.at[:, cols_of(q)]) for q in (px, py, pd)),
        )
    ):
        loads.append(pltpu.make_async_copy(src, dst, load_sem.at[min(i, 9)]))
    for i in (6, 0, 9, 10, 11, 1, 7, 8, 2, 3, 4, 5):
        loads[i].start()

    sends = []

    def send(src, dst, sem, there):
        copy = pltpu.make_async_remote_copy(
            src_ref=src,
            dst_ref=dst,
            send_sem=send_sem.at[0],
            recv_sem=sem,
            device_id=there,
            device_id_type=MESH,
        )
        copy.start()
        sends.append(math.prod(src.shape))

    def arrive(dst, sem):
        pltpu.make_async_remote_copy(
            src_ref=dst,
            dst_ref=dst,
            send_sem=send_sem.at[0],
            recv_sem=sem,
            device_id=to_x,
            device_id_type=MESH,
        ).wait_recv()

    with scope("hits"):
        loads[6].wait()
        rows_t = rows_ref[...].astype(f32).T
        lane = lax.broadcasted_iota(jnp.int32, (slot, tok_rows), 1).astype(f32)
        hits = jnp.concatenate(
            [jnp.where(rows_t[:, k : k + 1] == lane, 1.0, 0.0) for k in range(n_ep)], axis=0
        )
        chosen = hits.astype(bf16)
        loads[0].wait()
    with scope("pick"):
        pick[:, own] = dot(chosen, tok[:, own]).astype(bf16)
    with scope("barrier"):
        pl.semaphore_wait(barrier, n_ep + 1)

    def slot_of(pos):
        return pl.ds(pl.multiple_of(pos * slot, slot), slot)

    for g in (near, late):
        for c in range(2):
            peer = 2 * chips[g] + c
            pos = 2 * (near + inner) + core
            dst = xin.at[slot_of(pos), own]
            send(pick.at[block(peer), own], dst, z_sem.at[near + inner], {"ep": peer})
    with scope("pick2"):
        rest = tok.at[:, pl.ds(0, tok.shape[1] - width)]
        pltpu.make_async_copy(rest, rest, load_sem.at[9]).wait()
        for q in (px, py, pd):
            pick[:, cols_of(q)] = dot(chosen, tok[:, cols_of(q)]).astype(bf16)
    send(pick.at[block(partner)], xin.at[at(1)], z_sem.at[0], {"ep": partner})
    for c in range(2):
        peer = 2 * chips[mate] + c
        pos = 2 * mate + core
        send(pick.at[block(peer)], xin.at[slot_of(pos)], z_sem.at[mate], {"ep": peer})
    with scope("dhid"):
        loads[1].wait()
        dhid[p] = silu(dot(tok[...], w_side[...])).astype(bf16)
    send(dhid.at[p], dhid.at[p], dh_sem.at[0], to_x)
    send(dhid.at[p], dhid.at[p], dh_sem.at[0], to_y)
    xin[at(0), :] = pick[block(e), :]

    def combine_weights():
        loads[7].wait()
        cw_t = cw_ref[...].T
        weight = jnp.concatenate([cw_t[:, k : k + 1] for k in range(n_ep)], axis=0)
        both = (hits * weight).T
        high = both.astype(bf16)
        comb[0] = high
        comb[1] = (both - high.astype(f32)).astype(bf16)

    tile = 2 * LANES

    def gate_up_part(g, count):
        rows = pl.ds(2 * g * slot, 2 * count * slot)
        for n in range(hid.shape[1] // tile):
            cols = pl.ds(n * tile, tile)
            for acc, w in ((g_acc, w_gate), (u_acc, w_up)):
                total = dot(xin[rows, own], w[own, cols])
                for q in (px, py):
                    total += dot(xin[rows, cols_of(q)], w[cols_of(q), cols])
                acc[rows, cols] = total

    def gate_up_rest(g, count):
        rows = pl.ds(2 * g * slot, 2 * count * slot)
        for n in range(hid.shape[1] // tile):
            cols = pl.ds(n * tile, tile)
            gate = g_acc[rows, cols] + dot(xin[rows, far], w_gate[far, cols])
            up = u_acc[rows, cols] + dot(xin[rows, far], w_up[far, cols])
            hid[rows, cols] = (silu(gate) * up).astype(bf16)

    def gate_up(g, count=1, tiles=None):
        rows = pl.ds(2 * g * slot, 2 * count * slot)
        for n in tiles or range(hid.shape[1] // tile):
            cols = pl.ds(n * tile, tile)
            gate = dot(xin[rows, :], w_gate[:, cols])
            up = dot(xin[rows, :], w_up[:, cols])
            hid[rows, cols] = (silu(gate) * up).astype(bf16)

    def down(g, count, *slots):
        rows = pl.ds(2 * g * slot, 2 * count * slot)
        for to in slots:
            q = (p, px, py, pd)[to]
            for n in range(width // tile):
                src = pl.ds(pl.multiple_of(q * width + n * tile, tile), tile)
                part[to, rows, pl.ds(n * tile, tile)] = dot(
                    hid[rows, :], w_down[:, src]
                ).astype(bf16)

    def both(g):
        return pl.ds(2 * g * slot, 2 * slot)

    def spread(g):
        even, odd = 2 * g, 2 * g + 1
        arrive(xin.at[both(g), own], z_sem.at[g])
        for pos, axis in ((even, 0), (odd, 1), (odd, 0), (even, 1)):
            ref = xin.at[at(pos), own]
            kind = (pos + axis) % 2
            send(ref, ref, ag_sem.at[kind, g - near], (to_x, to_y)[axis])

    def forward(g):
        arrive(xin.at[both(g), own], ag_sem.at[0, g - near])
        for pos, q, there in ((2 * g, px, to_y), (2 * g + 1, py, to_x)):
            ref = xin.at[at(pos), cols_of(q)]
            send(ref, ref, ag_sem.at[2, g - near], there)

    def gathered_xy(g):
        arrive(xin.at[both(g), own], ag_sem.at[1, g - near])

    def gathered_d(g):
        arrive(xin.at[both(g), far], ag_sem.at[2, g - near])

    def first(g):
        for pos, there in ((2 * g + 1, to_x), (2 * g, to_y)):
            send(part.at[3, at(pos)], d_in.at[at(pos)], d_sem.at[g], there)

    def direct(g):
        even, odd = at(2 * g), at(2 * g + 1)
        send(part.at[1, odd], rx.at[odd], sum_sem.at[g], to_x)
        send(part.at[2, even], ry.at[even], sum_sem.at[g], to_y)

    def joined(g):
        arrive(d_in.at[both(g)], d_sem.at[g])
        for pos, src, dst, there in ((2 * g, 1, rx, to_x), (2 * g + 1, 2, ry, to_y)):
            b = at(pos)
            pair[b, :] = (part[src, b, :].astype(f32) + d_in[b, :].astype(f32)).astype(bf16)
            send(pair.at[b], dst.at[b], sum_sem.at[g], there)

    def finish(g):
        arrive(d_in.at[pl.ds(0, 4 * slot)], sum_sem.at[g])
        for c in range(2):
            pos = 2 * g + c
            b = at(pos)
            total = (
                part[0, b, :].astype(f32) + rx[b, :].astype(f32) + ry[b, :].astype(f32)
            ).astype(bf16)
            if pos == 0:
                back[block(e), :] = total
            else:
                fin[b, :] = total
                owner = partner if g == 0 else 2 * chips[g] + c
                send(fin.at[b], back.at[block(e)], ret_sem.at[0], {"ep": owner})

    half = tok_rows // 2

    def dense_branch():
        arrive(dhid.at[pd], dh_sem.at[1])
        loads[5].wait()
        loads[8].wait()
        total = dot(dhid[0], w_dout[pl.ds(0, side)])
        for q in range(1, dhid.shape[0]):
            total += dot(dhid[q], w_dout[pl.ds(q * side, side)])
        logit = jnp.sum(
            tok[...].astype(f32) * dgate_ref[...].reshape(1, tok.shape[1]).astype(f32),
            axis=1,
            keepdims=True,
        )
        dense[...] = total / (1.0 + jnp.exp(-logit))

    with scope("in0"):
        arrive(xin.at[at(1)], z_sem.at[0])
        loads[2].wait()
        loads[3].wait()
    n_tiles = hid.shape[1] // tile
    with scope("gu0a"):
        gate_up(0, 1, range(n_tiles // 2))
    with scope("gu0b"):
        gate_up(0, 1, range(n_tiles // 2, n_tiles))
    with scope("down0"):
        loads[4].wait()
        down(0, 1, 3)
        first(0)
        down(0, 1, 1, 2)
        direct(0)
        down(0, 1, 0)
    with scope("spreadA"):
        spread(near)
    with scope("comb"):
        combine_weights()
    with scope("spreadB"):
        spread(late)
    with scope("fwdA"):
        forward(near)
    with scope("join0"):
        joined(0)
    with scope("fwdB"):
        forward(late)
    with scope("dh_fwd"):
        arrive(dhid.at[pl.ds(0, 2)], dh_sem.at[0])
        ref = dhid.at[px, pl.ds(0, half)]
        send(ref, ref, dh_sem.at[1], to_y)
        ref = dhid.at[py, pl.ds(half, half)]
        send(ref, ref, dh_sem.at[1], to_x)
    with scope("inAxy"):
        gathered_xy(near)
    with scope("guAp"):
        gate_up_part(near, 1)
    with scope("inP"):
        arrive(xin.at[both(mate)], z_sem.at[mate])
    with scope("inBxy"):
        gathered_xy(late)
    with scope("guBp"):
        gate_up_part(late, 2)
    with scope("inAd"):
        gathered_d(near)
    with scope("guAr"):
        gate_up_rest(near, 1)
    with scope("downA"):
        down(near, 1, 3)
        first(near)
        down(near, 1, 1, 2)
        direct(near)
    with scope("inBd"):
        gathered_d(late)
    with scope("guBr"):
        gate_up_rest(late, 2)
    with scope("downB"):
        down(late, 2, 3)
        first(mate)
        first(late)
        down(late, 2, 1, 2)
        down(near, 1, 0)
    with scope("joinA"):
        joined(near)
    direct(mate)
    with scope("downB0"):
        down(late, 2, 0)
    with scope("joinP"):
        joined(mate)
    direct(late)
    with scope("joinB"):
        joined(late)
    with scope("finA"):
        finish(near)
    with scope("fin0"):
        finish(0)
    with scope("finP"):
        finish(mate)
    with scope("finB"):
        finish(late)
    with scope("dense"):
        dense_branch()
    with scope("ret"):
        arrive(back.at[pl.ds(0, (n_ep - 1) * slot)], ret_sem.at[0])
    with scope("out"):
        out_ref[...] = (
            dense[...] + dot(comb[0], back[...]) + dot(comb[1], back[...])
        ).astype(bf16)
    with scope("drain"):
        sent = w_gate.at[pl.ds(0, sum(sends) // w_gate.shape[1])]
        pltpu.make_async_copy(sent, sent, send_sem.at[0]).wait()


def fused_per_device(
    tokens,
    gate_proj,
    up_proj,
    down_proj,
    side_input_weight,
    dense_out,
    dense_gate,
    chosen_rows,
    choice_weights,
):
    n_ep, slot = chosen_rows.shape
    n_tp = lax.axis_size("tp")
    tok_rows, d = tokens.shape
    width = d // n_tp
    ff = gate_proj.shape[2]
    side = side_input_weight.shape[1]
    cap = n_ep * slot
    bf16, f32 = jnp.bfloat16, jnp.float32
    hbm = pl.BlockSpec(memory_space=pltpu.HBM)
    vmem = pl.BlockSpec(memory_space=pltpu.VMEM)
    return pl.pallas_call(
        functools.partial(layer_kernel, slot),
        out_shape=pltpu.VMEM((tok_rows, width), bf16),
        in_specs=[hbm] * 9,
        out_specs=vmem,
        scratch_shapes=[
            pltpu.VMEM(dense_gate.shape, bf16),
            pltpu.VMEM(chosen_rows.shape, jnp.int32),
            pltpu.VMEM(choice_weights.shape, f32),
            pltpu.VMEM((tok_rows, d), bf16),
            pltpu.VMEM((d, ff), bf16),
            pltpu.VMEM((d, ff), bf16),
            pltpu.VMEM((ff, d), bf16),
            pltpu.VMEM((d, side), bf16),
            pltpu.VMEM((n_tp * side, width), bf16),
            pltpu.VMEM((cap, d), bf16),
            pltpu.VMEM((cap, d), bf16),
            pltpu.VMEM((cap, ff), f32),
            pltpu.VMEM((cap, ff), f32),
            pltpu.VMEM((cap, ff), bf16),
            pltpu.VMEM((2, tok_rows, cap), bf16),
            pltpu.VMEM((n_tp, tok_rows, side), bf16),
            pltpu.VMEM((tok_rows, width), f32),
            pltpu.VMEM((4, cap, width), bf16),
            pltpu.VMEM((cap, width), bf16),
            pltpu.VMEM((cap, width), bf16),
            pltpu.VMEM((cap, width), bf16),
            pltpu.VMEM((cap, width), bf16),
            pltpu.VMEM((cap, width), bf16),
            pltpu.VMEM((cap, width), bf16),
            pltpu.SemaphoreType.DMA((10,)),
            pltpu.SemaphoreType.DMA((1,)),
            pltpu.SemaphoreType.DMA((4,)),
            pltpu.SemaphoreType.DMA((3, 2)),
            pltpu.SemaphoreType.DMA((2,)),
            pltpu.SemaphoreType.DMA((4,)),
            pltpu.SemaphoreType.DMA((4,)),
            pltpu.SemaphoreType.DMA((1,)),
        ],
        compiler_params=pltpu.CompilerParams(collective_id=0, has_side_effects=True),
    )(
        tokens,
        gate_proj,
        up_proj,
        down_proj,
        side_input_weight,
        dense_out,
        dense_gate,
        chosen_rows,
        choice_weights,
    )


def per_device(*args):
    tokens, gate_proj, chosen_rows = args[0], args[1], args[7]
    n_ep, slot = chosen_rows.shape
    n_tp = lax.axis_size("tp")
    width, tile = tokens.shape[1] // n_tp, 2 * LANES
    fits = (
        n_tp == 4
        and n_ep == 8
        and tokens.shape[0] == n_ep * slot
        and slot % 16 == 0
        and width % tile == 0
        and gate_proj.shape[2] == 2 * width
        and args[4].shape[1] % LANES == 0
        and 2 * args[4].shape[1] == width
    )
    return fused_per_device(*args) if fits else plain_per_device(*args)


def solution(mesh):
    placed = (
        P("ep", None),
        P("ep", None, "tp"),
        P("ep", None, "tp"),
        P("ep", "tp", None),
        P(None, "tp"),
        P(None, "tp"),
        P(),
        P(None, "ep"),
        P(None, "ep"),
    )
    return jax.shard_map(
        per_device, mesh=mesh, in_specs=placed, out_specs=P("ep", "tp"), check_vma=False
    )
```

```python
import functools
import math

import jax
import jax.numpy as jnp
from jax import lax
from jax.experimental import pallas as pl
from jax.experimental.pallas import tpu as pltpu
from jax.sharding import PartitionSpec as P

MESH = pl.DeviceIdType.MESH
LANES = 128


def plain_per_device(
    tokens,
    gate_proj,
    up_proj,
    down_proj,
    side_input_weight,
    dense_out,
    dense_gate,
    chosen_rows,
    choice_weights,
):
    tok_rows = tokens.shape[0]
    width = tokens.shape[1] // lax.axis_size("tp")
    column_position = lax.axis_index("tp") * width
    own_cols = lax.dynamic_slice_in_dim(tokens, column_position, width, 1)
    expert_count, slot_rows = chosen_rows.shape
    capacity = expert_count * slot_rows
    picked = jnp.take(own_cols, chosen_rows.reshape(-1), axis=0).reshape(
        expert_count, slot_rows, width
    )
    arrived = lax.all_to_all(picked, "ep", split_axis=0, concat_axis=1, tiled=True).reshape(
        capacity, width
    )
    piece = lax.all_gather(arrived, "tp", axis=1, tiled=True)
    gate_val = jnp.dot(piece, gate_proj[0], preferred_element_type=jnp.float32)
    up_val = jnp.dot(piece, up_proj[0], preferred_element_type=jnp.float32)
    hidden = (jax.nn.silu(gate_val) * up_val).astype(jnp.bfloat16)
    summed = lax.psum_scatter(
        lax.dot_general(
            down_proj[0], hidden, (((0,), (1,)), ((), ())), preferred_element_type=jnp.float32
        ).astype(jnp.bfloat16),
        "tp",
        scatter_dimension=0,
        tiled=True,
    )
    returned = lax.all_to_all(summed, "ep", split_axis=1, concat_axis=1, tiled=True)
    hits = (
        chosen_rows.reshape(-1)[:, None] == jnp.arange(tok_rows, dtype=jnp.int32)[None, :]
    ).astype(jnp.bfloat16)
    scaled = returned.astype(jnp.float32) * choice_weights.reshape(-1)[None, :]
    high_part = scaled.astype(jnp.bfloat16)
    lower_half = (scaled - high_part.astype(jnp.float32)).astype(jnp.bfloat16)
    contract = (((0,), (1,)), ((), ()))
    routed = lax.dot_general(
        hits, high_part, contract, preferred_element_type=jnp.float32
    ) + lax.dot_general(hits, lower_half, contract, preferred_element_type=jnp.float32)
    dense_hidden = jax.nn.silu(
        jnp.dot(tokens, side_input_weight, preferred_element_type=jnp.float32)
    ).astype(jnp.bfloat16)
    dense_val = jnp.dot(
        lax.all_gather(dense_hidden, "tp", axis=1, tiled=True),
        dense_out,
        preferred_element_type=jnp.float32,
    )
    side_gate = jax.nn.sigmoid(jnp.dot(tokens, dense_gate, preferred_element_type=jnp.float32))
    return (routed + side_gate[:, None] * dense_val).astype(jnp.bfloat16)


def dot(a, b):
    return jnp.dot(a, b, preferred_element_type=jnp.float32)


def silu(v):
    return v / (1.0 + jnp.exp(-v))


def layer_kernel(
    slot,
    tok_hbm,
    gate_hbm,
    up_hbm,
    down_hbm,
    side_hbm,
    dout_hbm,
    dgate_hbm,
    rows_hbm,
    cw_hbm,
    out_ref,
    dgate_ref,
    rows_ref,
    cw_ref,
    tok,
    w_gate,
    w_up,
    w_down,
    w_side,
    w_dout,
    pick,
    xin,
    g_acc,
    u_acc,
    hid,
    comb,
    dhid,
    dense,
    part,
    d_in,
    rx,
    ry,
    pair,
    fin,
    back,
    load_sem,
    send_sem,
    z_sem,
    ag_sem,
    dh_sem,
    d_sem,
    sum_sem,
    ret_sem,
):
    n_ep = rows_ref.shape[0]
    e = lax.axis_index("ep")
    p = lax.axis_index("tp")
    px = p + 1 - 2 * (p % 2)
    py = p + 2 - 4 * (p // 2)
    pd = px + 2 - 4 * (px // 2)
    z = e // 2
    core = e % 2
    partner = e + 1 - 2 * core
    upper = z // 2
    inner = (z + upper) % 2
    chips = [z, 3 - 3 * upper, 2 - upper, z + 1 - 2 * (z % 2)]
    near, late, mate = 1, 2, 3
    width = out_ref.shape[1]
    tok_rows = tok.shape[0]
    side = w_side.shape[1]
    to_x, to_y = {"tp": px}, {"tp": py}
    f32, bf16 = jnp.float32, jnp.bfloat16
    scope = jax.named_scope

    def block(owner):
        return pl.ds(pl.multiple_of(owner * slot, slot), slot)

    def at(pos):
        return pl.ds(pos * slot, slot)

    def cols_of(q):
        return pl.ds(pl.multiple_of(q * width, width), width)

    own, far = cols_of(p), cols_of(pd)

    barrier = pltpu.get_barrier_semaphore()
    for k in range(1, n_ep):
        pl.semaphore_signal(
            barrier, inc=1, device_id={"ep": (e + k) % n_ep}, device_id_type=MESH
        )
    for there in (to_x, to_y):
        pl.semaphore_signal(barrier, inc=1, device_id=there, device_id_type=MESH)

    loads = []
    for i, (src, dst) in enumerate(
        (
            (tok_hbm.at[:, own], tok.at[:, own]),
            (side_hbm, w_side),
            (gate_hbm.at[0], w_gate),
            (up_hbm.at[0], w_up),
            (down_hbm.at[0], w_down),
            (dout_hbm, w_dout),
            (rows_hbm, rows_ref),
            (cw_hbm, cw_ref),
            (dgate_hbm, dgate_ref),
            *((tok_hbm.at[:, cols_of(q)], tok.at[:, cols_of(q)]) for q in (px, py, pd)),
        )
    ):
        loads.append(pltpu.make_async_copy(src, dst, load_sem.at[min(i, 9)]))
    for i in (6, 0, 9, 10, 11, 1, 7, 8, 2, 3, 4, 5):
        loads[i].start()

    sends = []

    def send(src, dst, sem, there):
        copy = pltpu.make_async_remote_copy(
            src_ref=src,
            dst_ref=dst,
            send_sem=send_sem.at[0],
            recv_sem=sem,
            device_id=there,
            device_id_type=MESH,
        )
        copy.start()
        sends.append(math.prod(src.shape))

    def arrive(dst, sem):
        pltpu.make_async_remote_copy(
            src_ref=dst,
            dst_ref=dst,
            send_sem=send_sem.at[0],
            recv_sem=sem,
            device_id=to_x,
            device_id_type=MESH,
        ).wait_recv()

    with scope("hits"):
        loads[6].wait()
        rows_t = rows_ref[...].astype(f32).T
        lane = lax.broadcasted_iota(jnp.int32, (slot, tok_rows), 1).astype(f32)
        hits = jnp.concatenate(
            [jnp.where(rows_t[:, k : k + 1] == lane, 1.0, 0.0) for k in range(n_ep)], axis=0
        )
        chosen = hits.astype(bf16)
        loads[0].wait()
    with scope("pick"):
        pick[:, own] = dot(chosen, tok[:, own]).astype(bf16)
    with scope("barrier"):
        pl.semaphore_wait(barrier, n_ep + 1)

    def slot_of(pos):
        return pl.ds(pl.multiple_of(pos * slot, slot), slot)

    for g in (near, late):
        for c in range(2):
            peer = 2 * chips[g] + c
            pos = 2 * (near + inner) + core
            dst = xin.at[slot_of(pos), own]
            send(pick.at[block(peer), own], dst, z_sem.at[near + inner], {"ep": peer})
    with scope("pick2"):
        rest = tok.at[:, pl.ds(0, tok.shape[1] - width)]
        pltpu.make_async_copy(rest, rest, load_sem.at[9]).wait()
        for q in (px, py, pd):
            pick[:, cols_of(q)] = dot(chosen, tok[:, cols_of(q)]).astype(bf16)
    send(pick.at[block(partner)], xin.at[at(1)], z_sem.at[0], {"ep": partner})
    for c in range(2):
        peer = 2 * chips[mate] + c
        pos = 2 * mate + core
        send(pick.at[block(peer)], xin.at[slot_of(pos)], z_sem.at[mate], {"ep": peer})
    with scope("dhid"):
        loads[1].wait()
        dhid[p] = silu(dot(tok[...], w_side[...])).astype(bf16)
    send(dhid.at[p], dhid.at[p], dh_sem.at[0], to_x)
    send(dhid.at[p], dhid.at[p], dh_sem.at[0], to_y)
    xin[at(0), :] = pick[block(e), :]

    def combine_weights():
        loads[7].wait()
        cw_t = cw_ref[...].T
        weight = jnp.concatenate([cw_t[:, k : k + 1] for k in range(n_ep)], axis=0)
        both = (hits * weight).T
        high = both.astype(bf16)
        comb[0] = high
        comb[1] = (both - high.astype(f32)).astype(bf16)

    tile = 2 * LANES

    def gate_up_part(g, count):
        rows = pl.ds(2 * g * slot, 2 * count * slot)
        for n in range(hid.shape[1] // tile):
            cols = pl.ds(n * tile, tile)
            for acc, w in ((g_acc, w_gate), (u_acc, w_up)):
                total = dot(xin[rows, own], w[own, cols])
                for q in (px, py):
                    total += dot(xin[rows, cols_of(q)], w[cols_of(q), cols])
                acc[rows, cols] = total

    def gate_up_rest(g, count):
        rows = pl.ds(2 * g * slot, 2 * count * slot)
        for n in range(hid.shape[1] // tile):
            cols = pl.ds(n * tile, tile)
            gate = g_acc[rows, cols] + dot(xin[rows, far], w_gate[far, cols])
            up = u_acc[rows, cols] + dot(xin[rows, far], w_up[far, cols])
            hid[rows, cols] = (silu(gate) * up).astype(bf16)

    def gate_up(g, count=1, tiles=None):
        rows = pl.ds(2 * g * slot, 2 * count * slot)
        for n in tiles or range(hid.shape[1] // tile):
            cols = pl.ds(n * tile, tile)
            gate = dot(xin[rows, :], w_gate[:, cols])
            up = dot(xin[rows, :], w_up[:, cols])
            hid[rows, cols] = (silu(gate) * up).astype(bf16)

    def down(g, count, *slots):
        rows = pl.ds(2 * g * slot, 2 * count * slot)
        for to in slots:
            q = (p, px, py, pd)[to]
            for n in range(width // tile):
                src = pl.ds(pl.multiple_of(q * width + n * tile, tile), tile)
                part[to, rows, pl.ds(n * tile, tile)] = dot(
                    hid[rows, :], w_down[:, src]
                ).astype(bf16)

    def both(g):
        return pl.ds(2 * g * slot, 2 * slot)

    def spread(g):
        even, odd = 2 * g, 2 * g + 1
        arrive(xin.at[both(g), own], z_sem.at[g])
        for pos, axis in ((even, 0), (odd, 1), (odd, 0), (even, 1)):
            ref = xin.at[at(pos), own]
            kind = (pos + axis) % 2
            send(ref, ref, ag_sem.at[kind, g - near], (to_x, to_y)[axis])

    def forward(g):
        arrive(xin.at[both(g), own], ag_sem.at[0, g - near])
        for pos, q, there in ((2 * g, px, to_y), (2 * g + 1, py, to_x)):
            ref = xin.at[at(pos), cols_of(q)]
            send(ref, ref, ag_sem.at[2, g - near], there)

    def gathered_xy(g):
        arrive(xin.at[both(g), own], ag_sem.at[1, g - near])

    def gathered_d(g):
        arrive(xin.at[both(g), far], ag_sem.at[2, g - near])

    def first(g):
        for pos, there in ((2 * g + 1, to_x), (2 * g, to_y)):
            send(part.at[3, at(pos)], d_in.at[at(pos)], d_sem.at[g], there)

    def direct(g):
        even, odd = at(2 * g), at(2 * g + 1)
        send(part.at[1, odd], rx.at[odd], sum_sem.at[g], to_x)
        send(part.at[2, even], ry.at[even], sum_sem.at[g], to_y)

    def joined(g):
        arrive(d_in.at[both(g)], d_sem.at[g])
        for pos, src, dst, there in ((2 * g, 1, rx, to_x), (2 * g + 1, 2, ry, to_y)):
            b = at(pos)
            pair[b, :] = (part[src, b, :].astype(f32) + d_in[b, :].astype(f32)).astype(bf16)
            send(pair.at[b], dst.at[b], sum_sem.at[g], there)

    def finish(g):
        arrive(d_in.at[pl.ds(0, 4 * slot)], sum_sem.at[g])
        for c in range(2):
            pos = 2 * g + c
            b = at(pos)
            total = (
                part[0, b, :].astype(f32) + rx[b, :].astype(f32) + ry[b, :].astype(f32)
            ).astype(bf16)
            if pos == 0:
                back[block(e), :] = total
            else:
                fin[b, :] = total
                owner = partner if g == 0 else 2 * chips[g] + c
                send(fin.at[b], back.at[block(e)], ret_sem.at[0], {"ep": owner})

    half = tok_rows // 2

    def dense_branch():
        arrive(dhid.at[pd], dh_sem.at[1])
        loads[5].wait()
        loads[8].wait()
        total = dot(dhid[0], w_dout[pl.ds(0, side)])
        for q in range(1, dhid.shape[0]):
            total += dot(dhid[q], w_dout[pl.ds(q * side, side)])
        logit = jnp.sum(
            tok[...].astype(f32) * dgate_ref[...].reshape(1, tok.shape[1]).astype(f32),
            axis=1,
            keepdims=True,
        )
        dense[...] = total / (1.0 + jnp.exp(-logit))

    with scope("in0"):
        arrive(xin.at[at(1)], z_sem.at[0])
        loads[2].wait()
        loads[3].wait()
    n_tiles = hid.shape[1] // tile
    with scope("gu0a"):
        gate_up(0, 1, range(n_tiles // 2))
    with scope("gu0b"):
        gate_up(0, 1, range(n_tiles // 2, n_tiles))
    with scope("down0"):
        loads[4].wait()
        down(0, 1, 3)
        first(0)
        down(0, 1, 1, 2)
        direct(0)
        down(0, 1, 0)
    with scope("spreadA"):
        spread(near)
    with scope("comb"):
        combine_weights()
    with scope("spreadB"):
        spread(late)
    with scope("fwdA"):
        forward(near)
    with scope("join0"):
        joined(0)
    with scope("fwdB"):
        forward(late)
    with scope("dh_fwd"):
        arrive(dhid.at[pl.ds(0, 2)], dh_sem.at[0])
        ref = dhid.at[px, pl.ds(0, half)]
        send(ref, ref, dh_sem.at[1], to_y)
        ref = dhid.at[py, pl.ds(half, half)]
        send(ref, ref, dh_sem.at[1], to_x)
    with scope("inAxy"):
        gathered_xy(near)
    with scope("guAp"):
        gate_up_part(near, 1)
    with scope("inP"):
        arrive(xin.at[both(mate)], z_sem.at[mate])
    with scope("inBxy"):
        gathered_xy(late)
    with scope("guBp"):
        gate_up_part(late, 2)
    with scope("inAd"):
        gathered_d(near)
    with scope("guAr"):
        gate_up_rest(near, 1)
    with scope("downA"):
        down(near, 1, 3)
        first(near)
        down(near, 1, 1, 2)
        direct(near)
    with scope("inBd"):
        gathered_d(late)
    with scope("guBr"):
        gate_up_rest(late, 2)
    with scope("downB"):
        down(late, 2, 3)
        first(mate)
        first(late)
        down(late, 2, 1, 2)
    with scope("joinA"):
        joined(near)
    direct(mate)
    with scope("downB0"):
        down(near, 1, 0)
        down(late, 2, 0)
    direct(late)
    with scope("joinP"):
        joined(mate)
    with scope("joinB"):
        joined(late)
    with scope("finA"):
        finish(near)
    with scope("fin0"):
        finish(0)
    with scope("finP"):
        finish(mate)
    with scope("finB"):
        finish(late)
    with scope("dense"):
        dense_branch()
    with scope("ret"):
        arrive(back.at[pl.ds(0, (n_ep - 1) * slot)], ret_sem.at[0])
    with scope("out"):
        out_ref[...] = (
            dense[...] + dot(comb[0], back[...]) + dot(comb[1], back[...])
        ).astype(bf16)
    with scope("drain"):
        sent = w_gate.at[pl.ds(0, sum(sends) // w_gate.shape[1])]
        pltpu.make_async_copy(sent, sent, send_sem.at[0]).wait()


def fused_per_device(
    tokens,
    gate_proj,
    up_proj,
    down_proj,
    side_input_weight,
    dense_out,
    dense_gate,
    chosen_rows,
    choice_weights,
):
    n_ep, slot = chosen_rows.shape
    n_tp = lax.axis_size("tp")
    tok_rows, d = tokens.shape
    width = d // n_tp
    ff = gate_proj.shape[2]
    side = side_input_weight.shape[1]
    cap = n_ep * slot
    bf16, f32 = jnp.bfloat16, jnp.float32
    hbm = pl.BlockSpec(memory_space=pltpu.HBM)
    vmem = pl.BlockSpec(memory_space=pltpu.VMEM)
    return pl.pallas_call(
        functools.partial(layer_kernel, slot),
        out_shape=pltpu.VMEM((tok_rows, width), bf16),
        in_specs=[hbm] * 9,
        out_specs=vmem,
        scratch_shapes=[
            pltpu.VMEM(dense_gate.shape, bf16),
            pltpu.VMEM(chosen_rows.shape, jnp.int32),
            pltpu.VMEM(choice_weights.shape, f32),
            pltpu.VMEM((tok_rows, d), bf16),
            pltpu.VMEM((d, ff), bf16),
            pltpu.VMEM((d, ff), bf16),
            pltpu.VMEM((ff, d), bf16),
            pltpu.VMEM((d, side), bf16),
            pltpu.VMEM((n_tp * side, width), bf16),
            pltpu.VMEM((cap, d), bf16),
            pltpu.VMEM((cap, d), bf16),
            pltpu.VMEM((cap, ff), f32),
            pltpu.VMEM((cap, ff), f32),
            pltpu.VMEM((cap, ff), bf16),
            pltpu.VMEM((2, tok_rows, cap), bf16),
            pltpu.VMEM((n_tp, tok_rows, side), bf16),
            pltpu.VMEM((tok_rows, width), f32),
            pltpu.VMEM((4, cap, width), bf16),
            pltpu.VMEM((cap, width), bf16),
            pltpu.VMEM((cap, width), bf16),
            pltpu.VMEM((cap, width), bf16),
            pltpu.VMEM((cap, width), bf16),
            pltpu.VMEM((cap, width), bf16),
            pltpu.VMEM((cap, width), bf16),
            pltpu.SemaphoreType.DMA((10,)),
            pltpu.SemaphoreType.DMA((1,)),
            pltpu.SemaphoreType.DMA((4,)),
            pltpu.SemaphoreType.DMA((3, 2)),
            pltpu.SemaphoreType.DMA((2,)),
            pltpu.SemaphoreType.DMA((4,)),
            pltpu.SemaphoreType.DMA((4,)),
            pltpu.SemaphoreType.DMA((1,)),
        ],
        compiler_params=pltpu.CompilerParams(collective_id=0, has_side_effects=True),
    )(
        tokens,
        gate_proj,
        up_proj,
        down_proj,
        side_input_weight,
        dense_out,
        dense_gate,
        chosen_rows,
        choice_weights,
    )


def per_device(*args):
    tokens, gate_proj, chosen_rows = args[0], args[1], args[7]
    n_ep, slot = chosen_rows.shape
    n_tp = lax.axis_size("tp")
    width, tile = tokens.shape[1] // n_tp, 2 * LANES
    fits = (
        n_tp == 4
        and n_ep == 8
        and tokens.shape[0] == n_ep * slot
        and slot % 16 == 0
        and width % tile == 0
        and gate_proj.shape[2] == 2 * width
        and args[4].shape[1] % LANES == 0
        and 2 * args[4].shape[1] == width
    )
    return fused_per_device(*args) if fits else plain_per_device(*args)


def solution(mesh):
    placed = (
        P("ep", None),
        P("ep", None, "tp"),
        P("ep", None, "tp"),
        P("ep", "tp", None),
        P(None, "tp"),
        P(None, "tp"),
        P(),
        P(None, "ep"),
        P(None, "ep"),
    )
    return jax.shard_map(
        per_device, mesh=mesh, in_specs=placed, out_specs=P("ep", "tp"), check_vma=False
    )
```
